32 devices in a mesh: sp: 4 (over x, core), tp: 8 (over z, y).
Axes of the slice: x: 2, y: 2, z: 4, core: 2. Of those that a mesh axis runs over, the one named last changes fastest.
Arguments:
- latents: bfloat16 [1024, 2048], P(('sp', 'tp')), may hold values from -6 to 6
- context: bfloat16 [256, 2048], P('sp'), may hold values from -6 to 6
- condition: float32 [2048], P('sp'), may hold values from -12 to 12
- context_condition: float32 [2048], P('sp'), may hold values from -12 to 12
- norm_gain: float32 [2048], replicated, may hold values from 0.1 to 1.9
- shift_weight: bfloat16 [2048, 2048], P('sp', 'tp'), may hold values from -0.09375 to 0.09375
- scale_weight: bfloat16 [2048, 2048], P('sp', 'tp'), may hold values from -0.09375 to 0.09375
- gate_weight: bfloat16 [2048, 2048], P('sp', 'tp'), may hold values from -0.125 to 0.125
- query_weight: bfloat16 [2048, 1024], P(None, 'tp'), may hold values from -0.125 to 0.125
- key_weight: bfloat16 [2048, 1024], P(None, 'tp'), may hold values from -0.125 to 0.125
- value_weight: bfloat16 [2048, 1024], P(None, 'tp'), may hold values from -0.125 to 0.125
- subtract_share: float32 [8], P('tp'), may hold values from 0.3 to 0.8
- head_gain: float32 [128], replicated, may hold values from 0.1 to 1.9
- output_weight: bfloat16 [1024, 2048], P('tp'), may hold values from -0.1875 to 0.1875
Outputs:
- updated: bfloat16 [1024, 2048], P(('sp', 'tp'))
The draws below stay inside these ranges and needn't reach their ends.
All inputs are finite; a program needn't handle non-finite values.
Results may differ from the reference program's by a relative error of at most 0.013.
Values may be sent and summed in bfloat16 or wider, within the bound.
A program may use at most 64 MiB of HBM per device.

```python
import math
import jax
import jax.numpy as jnp
from jax import lax

D = 2048
HEAD = 64
VALUE = 128
HEADS = 8
GRID_W = 64
TOKENS = 1024
CTX = 256


def ramped_draw(base_key):
    position = jnp.arange(D, dtype=jnp.float32) / (D - 1)
    values = jnp.clip(jax.random.normal(base_key, (D,), jnp.float32), -4.0, 4.0)
    growth = jnp.exp(jnp.log(3.0) * position)
    return values * growth


def draw_condition(key, part):
    return ramped_draw(jax.random.fold_in(key, 11))


def draw_context_condition(key, part):
    return ramped_draw(jax.random.fold_in(key, 29))


def block_levels(key, shape, cuts, least, largest):
    def one(dim, shards_of):
        heights = jax.random.uniform(jax.random.fold_in(jax.random.fold_in(key, 6), dim), (shards_of,), jnp.float32, least / len(cuts), largest / len(cuts))
        return jnp.repeat(jnp.exp(heights), shape[dim] // shards_of).reshape((-1,) + (1,) * (len(shape) - dim - 1))

    level = one(*cuts[0])
    for cut in cuts[1:]:
        level = level * one(*cut)
    return level


def centred(rng, dims, spread, limit, cuts=(), kind=jnp.bfloat16):
    array = spread * jax.random.normal(rng, dims, jnp.float32)
    if cuts:
        array = array * block_levels(rng, dims, cuts, -0.22, 0.18)
    return jnp.clip(array, -limit, limit).astype(kind)


def setup_inputs(seed: int = 0) -> dict:
    streams_of = jax.random.split(jax.random.key(seed), 15)
    latents = centred(streams_of[0], (TOKENS, D), 1.0, 6.0, ((0, 32),))
    context = centred(streams_of[1], (CTX, D), 1.0, 6.0, ((0, 4),))
    condition = draw_condition(jax.random.fold_in(streams_of[14], 71), 0)
    context_condition = draw_context_condition(jax.random.fold_in(streams_of[14], 71), 0)
    norm_gain = jnp.clip(1.0 + 0.18 * jax.random.normal(streams_of[4], (D,), jnp.float32), 0.1, 1.9)
    shift_weight = centred(streams_of[5], (D, D), (2 * D) ** -0.5, 0.09375, ((0, 4), (1, 8)))
    scale_weight = centred(streams_of[6], (D, D), (2 * D) ** -0.5, 0.09375, ((0, 4), (1, 8)))
    gate_weight = centred(streams_of[7], (D, D), D ** -0.5, 0.125, ((0, 4), (1, 8)))
    query_weight = centred(streams_of[8], (D, HEADS * VALUE), D ** -0.5, 0.125, ((1, 8),))
    key_weight = centred(streams_of[9], (D, HEADS * VALUE), D ** -0.5, 0.125, ((1, 8),))
    value_weight = centred(streams_of[10], (D, HEADS * VALUE), D ** -0.5, 0.125, ((1, 8),))
    subtract_share = jnp.clip(0.3 + 0.5 * jax.random.uniform(streams_of[11], (HEADS,), jnp.float32) ** block_levels(streams_of[11], (HEADS,), ((0, 8),), -0.2, 0.2), 0.3, 0.8)
    head_gain = jnp.clip(1.0 + 0.18 * jax.random.normal(streams_of[12], (VALUE,), jnp.float32), 0.1, 1.9)
    output_weight = centred(streams_of[13], (HEADS * VALUE, D), (HEADS * VALUE) ** -0.5, 0.1875, ((0, 8),))
    return dict(latents=latents, context=context, condition=condition, context_condition=context_condition, norm_gain=norm_gain, shift_weight=shift_weight, scale_weight=scale_weight, gate_weight=gate_weight, query_weight=query_weight, key_weight=key_weight, value_weight=value_weight, subtract_share=subtract_share, head_gain=head_gain, output_weight=output_weight)


norm_eps = 1e-06
head_eps = 1e-05
rope_theta = 10000.0
head_scale = 0.8

def rotary_tables(positions):
    quarter = HEAD // 4
    inverse = rope_theta ** (-2.0 * jnp.arange(quarter, dtype=jnp.float32) / (HEAD // 2))
    row_angle = (positions // GRID_W).astype(jnp.float32)[:, None] * inverse[None, :]
    column_angle = (positions % GRID_W).astype(jnp.float32)[:, None] * inverse[None, :]
    angles = jnp.concatenate([row_angle, row_angle, column_angle, column_angle], axis=-1)
    return (jnp.cos(angles), jnp.sin(angles))

def rotate(vectors, cosine, sine_table):
    quarter = HEAD // 4
    pieces = vectors.reshape(vectors.shape[:-1] + (2, 2, quarter))
    turned = jnp.concatenate([-pieces[..., 1:, :], pieces[..., :1, :]], axis=-2).reshape(vectors.shape)
    return vectors * cosine[:, None, :] + turned * sine_table[:, None, :]

def modulate(token_rows, gain_row, shift_row, scale_row):
    widened = token_rows.astype(jnp.float32)
    normed = widened * lax.rsqrt(lax.optimization_barrier(jnp.mean(widened * widened, axis=-1, keepdims=True)) + norm_eps)
    return (normed * gain_row * (1.0 + scale_row) + shift_row).astype(jnp.bfloat16)

def differential(queries, key_value_rows, share_value, head_gain):
    ratios = []
    for which_map in range(2):
        offset = which_map * HEAD
        scores = jnp.dot(queries[:, offset:offset + HEAD], key_value_rows[:, offset:offset + HEAD].T, preferred_element_type=jnp.float32) * HEAD ** (-0.5)
        powers = jnp.exp(scores)
        weighted = jnp.dot(powers.astype(jnp.bfloat16), key_value_rows[:, VALUE:], preferred_element_type=jnp.float32)
        ratios.append(weighted / lax.optimization_barrier(jnp.sum(powers, axis=1, keepdims=True)))
    difference = ratios[0] - share_value * ratios[1]
    normed = difference * lax.rsqrt(lax.optimization_barrier(jnp.mean(difference * difference, axis=1, keepdims=True)) + head_eps)
    return (normed * head_gain * head_scale).astype(jnp.bfloat16)

def reference(latents, context, condition, context_condition, norm_gain, shift_weight, scale_weight, gate_weight, query_weight, key_weight, value_weight, subtract_share, head_gain, output_weight):
    activated = jax.nn.silu(jnp.stack([condition, context_condition])).astype(jnp.bfloat16)
    shift_terms = jnp.dot(activated, shift_weight, preferred_element_type=jnp.float32)
    scale_terms = jnp.dot(activated, scale_weight, preferred_element_type=jnp.float32)
    gate_terms = jnp.dot(activated, gate_weight, preferred_element_type=jnp.float32)
    latent_mod = modulate(latents, norm_gain, shift_terms[0], scale_terms[0])
    context_mod = modulate(context, norm_gain, shift_terms[1], scale_terms[1])
    cosine, sine_table = rotary_tables(jnp.arange(TOKENS, dtype=jnp.int32))
    block_rows = math.gcd(TOKENS, 512)

    def add_head(head_index, running):
        first_column = jnp.asarray(head_index, jnp.int32) * VALUE

        def columns(weight):
            return lax.dynamic_slice_in_dim(weight, first_column, VALUE, 1)
        latent_query = jnp.dot(latent_mod, columns(query_weight), preferred_element_type=jnp.float32)
        queries = rotate(latent_query.reshape(TOKENS, 2, HEAD), cosine, sine_table)
        queries = queries.reshape(TOKENS, VALUE).astype(jnp.bfloat16)
        latent_key = jnp.dot(latent_mod, columns(key_weight), preferred_element_type=jnp.float32)
        latent_keys = rotate(latent_key.reshape(TOKENS, 2, HEAD), cosine, sine_table)
        latent_keys = latent_keys.reshape(TOKENS, VALUE).astype(jnp.bfloat16)
        latent_values = jnp.dot(latent_mod, columns(value_weight), preferred_element_type=jnp.float32).astype(jnp.bfloat16)
        context_keys = jnp.dot(context_mod, columns(key_weight), preferred_element_type=jnp.float32).astype(jnp.bfloat16)
        context_values = jnp.dot(context_mod, columns(value_weight), preferred_element_type=jnp.float32).astype(jnp.bfloat16)
        key_value_rows = jnp.concatenate([jnp.concatenate([context_keys, context_values], axis=1), jnp.concatenate([latent_keys, latent_values], axis=1)], axis=0)
        share_value = lax.dynamic_index_in_dim(subtract_share, jnp.asarray(head_index, jnp.int32), 0, keepdims=False)

        def one_block(query_block):
            return differential(query_block, key_value_rows, share_value, head_gain)
        head_output = lax.map(one_block, queries.reshape(TOKENS // block_rows, block_rows, VALUE))
        head_output = head_output.reshape(TOKENS, VALUE)
        output_rows = lax.dynamic_slice_in_dim(output_weight, first_column, VALUE, 0)
        return running + jnp.dot(head_output, output_rows, preferred_element_type=jnp.float32)
    branch = lax.fori_loop(0, HEADS, add_head, jnp.zeros((TOKENS, D), jnp.float32))
    return (latents.astype(jnp.float32) + gate_terms[0] * branch).astype(jnp.bfloat16)
```

```python
import functools
import math

import jax
import jax.numpy as jnp
from jax import lax
from jax.experimental import pallas as pl
from jax.experimental.pallas import tpu as pltpu
from jax.sharding import PartitionSpec as P

HEAD = 64
VALUE = 128
GRID_W = 64


norm_eps = 1e-06
head_eps = 1e-05
rope_theta = 10000.0
head_scale = 0.8


def rotary_tables(positions):
    quarter = HEAD // 4
    inverse = rope_theta ** (-2.0 * jnp.arange(quarter, dtype=jnp.float32) / (HEAD // 2))
    row_angle = (positions // GRID_W).astype(jnp.float32)[:, None] * inverse[None, :]
    column_angle = (positions % GRID_W).astype(jnp.float32)[:, None] * inverse[None, :]
    angles = jnp.concatenate([row_angle, row_angle, column_angle, column_angle], axis=-1)
    return (jnp.cos(angles), jnp.sin(angles))


def rotate(vectors, cosine, sine_table):
    quarter = HEAD // 4
    pieces = vectors.reshape(vectors.shape[:-1] + (2, 2, quarter))
    turned = jnp.concatenate([-pieces[..., 1:, :], pieces[..., :1, :]], axis=-2).reshape(
        vectors.shape
    )
    return vectors * cosine[:, None, :] + turned * sine_table[:, None, :]


def modulate(token_rows, gain_row, shift_row, scale_row):
    widened = token_rows.astype(jnp.float32)
    normed = widened * lax.rsqrt(jnp.mean(widened * widened, axis=-1, keepdims=True) + norm_eps)
    return (normed * gain_row * (1.0 + scale_row) + shift_row).astype(jnp.bfloat16)


def shards(
    latents,
    context,
    condition,
    context_condition,
    norm_gain,
    shift_weight,
    scale_weight,
    gate_weight,
    query_weight,
    key_weight,
    value_weight,
    subtract_share,
    head_gain,
    output_weight,
):
    activated = jax.nn.silu(jnp.stack([condition, context_condition])).astype(jnp.bfloat16)
    partial_terms = jnp.stack(
        [
            jnp.dot(activated, matrix, preferred_element_type=jnp.float32)
            for matrix in (shift_weight, scale_weight, gate_weight)
        ]
    )
    summed = lax.psum(partial_terms, "sp")
    full_terms = lax.all_gather(summed, "tp", axis=2, tiled=True)
    shift_terms, scale_terms, gate_terms = (full_terms[0], full_terms[1], full_terms[2])
    pair_weight = jnp.concatenate([key_weight, value_weight], axis=1)
    joined = jnp.concatenate([query_weight, pair_weight], axis=1)
    projected = jnp.dot(
        modulate(
            lax.all_gather(latents, "tp", axis=0, tiled=True),
            norm_gain,
            shift_terms[0],
            scale_terms[0],
        ),
        joined,
        preferred_element_type=jnp.float32,
    )
    local_count = projected.shape[0]
    positions = lax.axis_index("sp") * local_count + jnp.arange(local_count, dtype=jnp.int32)
    cosine, sine_table = rotary_tables(positions)
    queries = rotate(projected[:, :VALUE].reshape(local_count, 2, HEAD), cosine, sine_table)
    queries = queries.reshape(local_count, VALUE).astype(jnp.bfloat16)
    latent_keys = rotate(
        projected[:, VALUE : 2 * VALUE].reshape(local_count, 2, HEAD), cosine, sine_table
    )
    latent_keys = latent_keys.reshape(local_count, VALUE).astype(jnp.bfloat16)
    latent_pairs = jnp.concatenate(
        [latent_keys, projected[:, 2 * VALUE :].astype(jnp.bfloat16)], axis=1
    )
    context_mod = modulate(context, norm_gain, shift_terms[1], scale_terms[1])
    context_pairs = jnp.dot(context_mod, pair_weight, preferred_element_type=jnp.float32).astype(
        jnp.bfloat16
    )
    sent_pairs = jnp.concatenate([latent_pairs, context_pairs], axis=0)
    arrived = lax.all_gather(sent_pairs, "sp", axis=0, tiled=True)
    updated_carry = []
    for which_map in range(2):
        offset = which_map * HEAD
        scores = jnp.einsum(
            "qd,kd->qk",
            queries[:, offset : offset + HEAD],
            arrived[:, offset : offset + HEAD],
            preferred_element_type=jnp.float32,
        ) * HEAD ** (-0.5)
        powers = jnp.exp(scores)
        updated_carry.append(
            jnp.dot(
                powers.astype(jnp.bfloat16), arrived[:, VALUE:], preferred_element_type=jnp.float32
            )
        )
        updated_carry.append(jnp.sum(powers, axis=1, keepdims=True))
    first_sum, first_total, second_sum, second_total = tuple(updated_carry)
    share_value = subtract_share[0]
    difference = first_sum / first_total - share_value * (second_sum / second_total)
    normed = difference * lax.rsqrt(
        jnp.mean(difference * difference, axis=1, keepdims=True) + head_eps
    )
    head_output = (normed * head_gain * head_scale).astype(jnp.bfloat16)
    branch = lax.psum_scatter(
        jnp.dot(head_output, output_weight, preferred_element_type=jnp.float32),
        "tp",
        scatter_dimension=0,
        tiled=True,
    )
    return (latents.astype(jnp.float32) + gate_terms[0] * branch).astype(jnp.bfloat16)


MESH = pl.DeviceIdType.MESH
CHUNKS = 2


def fused_kernel(
    lat_ref, ctx_ref, cond_ref, ccond_ref, gain_ref, shift_ref, scale_ref, gate_ref,
    wq_hbm, wk_hbm, wv_hbm, share_ref, hgain_ref, wo_hbm, out_ref,
    lat, mod, cmod, wqkv, wo, part, terms, tables, queries, kv, ho_send, ho,
    load_sem, lat_ss, lat_rs, part_ss, part_rs, term_ss, term_rs,
    kv_ss, kv_rs, ckv_ss, ckv_rs, ho_ss, ho_rs, wo_ss, wo_rs,
    *, S, T,
):
    f32, bf16 = jnp.float32, jnp.bfloat16
    rows, D = lat_ref.shape
    crows = ctx_ref.shape[0]
    count = rows * T
    width = D // T
    quarter_cols = D // S
    Z = T // 2
    i = lax.axis_index("sp")
    t = lax.axis_index("tp")
    z = lax.div(t, 2)
    y = lax.rem(t, 2)
    mate = t + 1 - 2 * y
    twin = i + 1 - 2 * lax.rem(i, 2)
    across = lax.rem(i + 2, S)
    twin_across = lax.rem(twin + 2, S)
    pending = []

    def when(cond, action):
        if cond is None:
            action()
        else:
            pl.when(cond)(action)

    def copy(src, dst, ss, rs, sp, tp):
        return pltpu.make_async_remote_copy(
            src_ref=src, dst_ref=dst, send_sem=ss, recv_sem=rs,
            device_id={"sp": sp, "tp": tp}, device_id_type=MESH,
        )

    def send(cond, src, dst, ss, rs, sp, tp):
        made = copy(src, dst, ss, rs, sp, tp)

        def go():
            made.start()

        when(cond, go)
        pending.append((cond, made))

    def arrived(dst, ss, rs):
        copy(dst, dst, ss, rs, twin, t).wait_recv()

    loads = [
        pltpu.make_async_copy(wq_hbm, wqkv.at[:, pl.ds(0, VALUE)], load_sem.at[0]),
        pltpu.make_async_copy(wk_hbm, wqkv.at[:, pl.ds(VALUE, VALUE)], load_sem.at[1]),
        pltpu.make_async_copy(wv_hbm, wqkv.at[:, pl.ds(2 * VALUE, VALUE)], load_sem.at[2]),
        pltpu.make_async_copy(wo_hbm, wo.at[pl.ds(t * VALUE, VALUE), :], load_sem.at[3]),
    ]
    for load in loads:
        load.start()

    barrier = pltpu.get_barrier_semaphore()
    for k in range(1, S):
        pl.semaphore_signal(
            barrier, inc=1, device_id={"sp": lax.rem(i + k, S), "tp": t}, device_id_type=MESH
        )
    for k in range(1, T):
        pl.semaphore_signal(
            barrier, inc=1, device_id={"sp": i, "tp": lax.rem(t + k, T)}, device_id_type=MESH
        )
    pl.semaphore_wait(barrier, S + T - 2)

    step = rows // CHUNKS

    def lat_piece(block, c):
        return lat.at[pl.ds(block * rows + c * step, step), :]

    for c in range(CHUNKS):
        own = lat_ref.at[pl.ds(c * step, step), :]
        dst = lat_piece(t, c)
        rs = lat_rs.at[c, t]
        send(z < Z - 1, own, dst, lat_ss.at[c, t, 0], rs, i, t + 2)
        send(z > 0, own, dst, lat_ss.at[c, t, 1], rs, i, t - 2)
        send(None, own, dst, lat_ss.at[c, t, 2], rs, i, mate)

    def lat_stage(d):
        for c in range(CHUNKS):
            for sign in (-1, 1):
                block = t + 2 * d * sign
                here = z - d >= 0 if sign < 0 else z + d < Z
                onward = jnp.logical_and(here, z < Z - 1 if sign < 0 else z > 0)
                piece = lat_piece(block, c)
                rs = lat_rs.at[c, block]

                def come(piece=piece, rs=rs, block=block, c=c):
                    arrived(piece, lat_ss.at[c, block, 0], rs)

                when(here, come)
                send(onward, piece, piece, lat_ss.at[c, block, 0], rs, i, t - 2 * sign)
                send(here, piece, piece, lat_ss.at[c, block, 2], rs, i, mate)

    def silu(v):
        return v / (1.0 + jnp.exp(-v))

    depth = cond_ref.shape[1]
    line = lax.broadcasted_iota(jnp.int32, (8, depth), 0)
    act0 = jnp.broadcast_to(silu(cond_ref[...]), (8, depth))
    act1 = jnp.broadcast_to(silu(ccond_ref[...]), (8, depth))

    def two_lines(first, matrix_ref, with_second):
        left = jnp.where(line == first, act0, 0.0)
        if with_second:
            left = jnp.where(line == first + 1, act1, left)
        return jnp.dot(left.astype(bf16), matrix_ref[...], preferred_element_type=f32)

    part[pl.ds(i, 1)] = (
        two_lines(0, shift_ref, True) + two_lines(2, scale_ref, True) + two_lines(4, gate_ref, False)
    )[None]
    for k in range(1, S):
        send(None, part.at[i], part.at[i], part_ss.at[k], part_rs.at[i], lax.rem(i + k, S), t)

    lat_stage(1)

    for k in range(1, S):
        peer = lax.rem(i + k, S)
        arrived(part.at[peer], part_ss.at[k], part_rs.at[peer])
    total = part[0]
    for k in range(1, S):
        total = total + part[k]
    terms[pl.ds(t, 1)] = total[None]
    for k in range(1, T):
        send(None, terms.at[t], terms.at[t], term_ss.at[k], term_rs.at[t], i, lax.rem(t + k, T))

    lane = lax.broadcasted_iota(jnp.int32, (count, VALUE), 1)
    place = i * count + lax.broadcasted_iota(jnp.int32, (count, VALUE), 0)
    spot = lax.rem(lane, HEAD)
    quarter = HEAD // 4
    power = lax.rem(spot, quarter).astype(f32) * (-2.0 / (HEAD // 2))
    inverse = jnp.exp(power * math.log(rope_theta))
    along = jnp.where(spot < HEAD // 2, lax.div(place, GRID_W), lax.rem(place, GRID_W))
    angle = along.astype(f32) * inverse
    even = lax.rem(lax.div(spot, quarter), 2) == 0
    tables[0] = jnp.cos(angle)
    tables[1] = jnp.sin(angle)

    for d in range(2, Z):
        lat_stage(d)

    loads[3].wait()

    def wo_piece(block, share):
        return wo.at[pl.ds(block * VALUE, VALUE), pl.ds(share * quarter_cols, quarter_cols)]

    own_wo = wo_piece(t, i)
    send(z < Z - 1, own_wo, own_wo, wo_ss.at[t, 0], wo_rs.at[t, i], i, t + 2)
    send(z > 0, own_wo, own_wo, wo_ss.at[t, 1], wo_rs.at[t, i], i, t - 2)
    send(None, own_wo, own_wo, wo_ss.at[t, 2], wo_rs.at[t, i], i, mate)

    def wo_side(cond, block):
        piece = wo_piece(block, i)
        send(cond, piece, piece, wo_ss.at[block, 3], wo_rs.at[block, i], across, t)
        send(cond, piece, piece, wo_ss.at[block, 4], wo_rs.at[block, i], twin, t)

    def wo_stage(d):
        for sign in (-1, 1):
            block = t + 2 * d * sign
            here = z - d >= 0 if sign < 0 else z + d < Z
            onward = jnp.logical_and(here, z < Z - 1 if sign < 0 else z > 0)
            piece = wo_piece(block, i)
            rs = wo_rs.at[block, i]

            def come(piece=piece, rs=rs, block=block):
                arrived(piece, wo_ss.at[block, 0], rs)

            when(here, come)
            send(onward, piece, piece, wo_ss.at[block, 0], rs, i, t - 2 * sign)
            send(here, piece, piece, wo_ss.at[block, 2], rs, i, mate)
            wo_side(here, block)

    def wo_mate(d):
        for sign in (-1, 1) if d else (1,):
            block = mate + 2 * d * sign
            here = None if not d else (z - d >= 0 if sign < 0 else z + d < Z)
            piece = wo_piece(block, i)

            def come(piece=piece, block=block):
                arrived(piece, wo_ss.at[block, 0], wo_rs.at[block, i])

            when(here, come)
            wo_side(here, block)

    def wo_across(column, d):
        for sign in (-1, 1) if d else (1,):
            block = column + 2 * d * sign
            here = None if not d else (z - d >= 0 if sign < 0 else z + d < Z)
            piece = wo_piece(block, across)

            def come(piece=piece, block=block):
                arrived(piece, wo_ss.at[block, 0], wo_rs.at[block, across])

            when(here, come)
            send(here, piece, piece, wo_ss.at[block, 5], wo_rs.at[block, across], twin, t)

    for k in range(1, T):
        peer = lax.rem(t + k, T)
        arrived(terms.at[peer], term_ss.at[k], term_rs.at[peer])

    def modulate_into(dst, src, first, n, which):
        wide = src[...].astype(f32)
        factor = lax.rsqrt(jnp.mean(wide * wide, axis=-1, keepdims=True) + norm_eps)
        for j in range(T):
            cols = slice(j * width, (j + 1) * width)
            mult = gain_ref[:, cols] * (1.0 + terms[j, 2 + which : 3 + which, :])
            shifted = wide[:, cols] * factor * mult + terms[j, which : which + 1, :]
            dst[pl.ds(first, n), cols] = shifted.astype(bf16)

    for load in loads[:3]:
        load.wait()
    modulate_into(cmod, ctx_ref, 0, crows, 1)
    kv[pl.ds(i, 1), pl.ds(count, crows), :] = jnp.dot(
        cmod[...], wqkv[:, VALUE:], preferred_element_type=f32
    ).astype(bf16)[None]

    def ckv_piece(s):
        return kv.at[s, pl.ds(count, crows), :]

    def kv_piece(s):
        return kv.at[s, pl.ds(0, count), :]

    send(None, ckv_piece(i), ckv_piece(i), ckv_ss.at[0], ckv_rs.at[i], across, t)
    send(None, ckv_piece(i), ckv_piece(i), ckv_ss.at[1], ckv_rs.at[i], twin, t)

    for d in range(Z):
        for sign in (-1, 1) if d else (1,):
            block = mate + 2 * d * sign
            here = None if not d else (z - d >= 0 if sign < 0 else z + d < Z)
            for c in range(CHUNKS):
                def come(block=block, c=c):
                    arrived(lat_piece(block, c), lat_ss.at[c, block, 0], lat_rs.at[c, block])

                when(here, come)
    lat[pl.ds(t * rows, rows), :] = lat_ref[...]
    modulate_into(mod, lat, 0, count, 0)
    projected = jnp.dot(mod[...], wqkv[...], preferred_element_type=f32)

    def rotated(u):
        turned = jnp.where(even, -pltpu.roll(u, VALUE - quarter, 1), pltpu.roll(u, quarter, 1))
        return u * tables[0] + turned * tables[1]

    kv[pl.ds(i, 1), pl.ds(0, count), pl.ds(0, VALUE)] = (
        rotated(projected[:, VALUE : 2 * VALUE]).astype(bf16)[None]
    )
    kv[pl.ds(i, 1), pl.ds(0, count), pl.ds(VALUE, VALUE)] = (
        projected[:, 2 * VALUE :].astype(bf16)[None]
    )
    send(None, kv_piece(i), kv_piece(i), kv_ss.at[0], kv_rs.at[i], across, t)
    send(None, kv_piece(i), kv_piece(i), kv_ss.at[1], kv_rs.at[i], twin, t)
    arrived(ckv_piece(across), ckv_ss.at[2], ckv_rs.at[across])
    send(None, ckv_piece(across), ckv_piece(across), ckv_ss.at[2], ckv_rs.at[across], twin, t)
    query = rotated(projected[:, :VALUE]).astype(bf16) * jnp.asarray(HEAD ** (-0.5), bf16)
    first_half = lane < HEAD
    zero = jnp.zeros_like(query)
    queries[0:count, :] = jnp.where(first_half, query, zero)
    queries[count:, :] = jnp.where(first_half, zero, query)
    wo_stage(1)
    wo_mate(0)

    ones = jnp.ones((count + crows, VALUE), bf16)

    def attend(slot):
        rows_kv = kv[slot]
        scores = lax.dot_general(
            queries[...], rows_kv[:, :VALUE], (((1,), (1,)), ((), ())), preferred_element_type=f32
        )
        return jnp.dot(
            jnp.exp(scores).astype(bf16),
            jnp.concatenate([rows_kv[:, VALUE:], ones], axis=1),
            preferred_element_type=f32,
        )

    sums = attend(i)
    wo_stage(2) if Z > 2 else None
    arrived(kv_piece(twin), kv_ss.at[2], kv_rs.at[twin])
    arrived(ckv_piece(twin), ckv_ss.at[2], ckv_rs.at[twin])
    sums = sums + attend(twin)
    wo_mate(1)
    arrived(kv_piece(across), kv_ss.at[2], kv_rs.at[across])
    send(None, kv_piece(across), kv_piece(across), kv_ss.at[2], kv_rs.at[across], twin, t)
    sums = sums + attend(across)
    arrived(kv_piece(twin_across), kv_ss.at[2], kv_rs.at[twin_across])
    arrived(ckv_piece(twin_across), ckv_ss.at[2], ckv_rs.at[twin_across])
    sums = sums + attend(twin_across)
    ratio = sums[:, :VALUE] / sums[:, VALUE:]
    difference = ratio[:count] - share_ref[0] * ratio[count:]
    normed = difference * lax.rsqrt(
        jnp.mean(difference * difference, axis=1, keepdims=True) + head_eps
    )
    ho_send[...] = (normed * hgain_ref[...] * head_scale).astype(bf16)
    for k in range(1, T):
        peer = lax.rem(t + k, T)
        send(
            None, ho_send.at[pl.ds(peer * rows, rows), :], ho.at[t], ho_ss.at[k], ho_rs.at[t], i, peer
        )
    ho[pl.ds(t, 1)] = ho_send[pl.ds(t * rows, rows), :][None]

    for d in range(3, Z):
        wo_stage(d)
    for d in range(2, Z):
        wo_mate(d)
    for d in range(Z):
        if d:
            wo_across(t, d)
        wo_across(mate, d)
    for k in range(1, T):
        peer = lax.rem(t + k, T)
        arrived(ho.at[peer], ho_ss.at[k], ho_rs.at[peer])
        for share in (twin, twin_across):
            arrived(wo_piece(peer, share), wo_ss.at[peer, 0], wo_rs.at[peer, share])
    heads = jnp.concatenate([ho[h] for h in range(T)], axis=1)
    for j in range(T):
        cols = slice(j * width, (j + 1) * width)
        branch = jnp.dot(heads, wo[:, cols], preferred_element_type=f32)
        out_ref[:, cols] = (
            lat_ref[:, cols].astype(f32) + terms[j, 4:5, :] * branch
        ).astype(bf16)

    for cond, made in pending:
        def finish(made=made):
            made.wait_send()

        when(cond, finish)


def fused_shards(S, T, *args):
    (latents, context, condition, context_condition, norm_gain, shift_weight, scale_weight,
     gate_weight, query_weight, key_weight, value_weight, subtract_share, head_gain,
     output_weight) = args
    rows, D = latents.shape
    crows = context.shape[0]
    count = rows * T
    bf16, f32 = jnp.bfloat16, jnp.float32
    vmem = pl.BlockSpec(memory_space=pltpu.VMEM)
    hbm = pl.BlockSpec(memory_space=pl.ANY)
    smem = pl.BlockSpec(memory_space=pltpu.SMEM)
    dma = pltpu.SemaphoreType.DMA
    return pl.pallas_call(
        functools.partial(fused_kernel, S=S, T=T),
        out_shape=jax.ShapeDtypeStruct((rows, D), bf16),
        in_specs=[vmem] * 8 + [hbm] * 3 + [smem, vmem, hbm],
        out_specs=vmem,
        scratch_shapes=[
            pltpu.VMEM((count, D), bf16),
            pltpu.VMEM((count, D), bf16),
            pltpu.VMEM((crows, D), bf16),
            pltpu.VMEM((D, 3 * VALUE), bf16),
            pltpu.VMEM((T * VALUE, D), bf16),
            pltpu.VMEM((S, 8, D // T), f32),
            pltpu.VMEM((T, 8, D // T), f32),
            pltpu.VMEM((2, count, VALUE), f32),
            pltpu.VMEM((2 * count, VALUE), bf16),
            pltpu.VMEM((S, count + crows, 2 * VALUE), bf16),
            pltpu.VMEM((count, VALUE), bf16),
            pltpu.VMEM((T, rows, VALUE), bf16),
            dma((4,)), dma((CHUNKS, T, 3)), dma((CHUNKS, T)), dma((S,)), dma((S,)),
            dma((T,)), dma((T,)), dma((3,)), dma((S,)), dma((3,)), dma((S,)),
            dma((T,)), dma((T,)), dma((T, 6)), dma((T, S)),
        ],
        compiler_params=pltpu.CompilerParams(
            collective_id=0, has_side_effects=True, vmem_limit_bytes=56 * 1024 * 1024
        ),
    )(latents, context, condition[None, :], context_condition[None, :], norm_gain[None, :],
      shift_weight, scale_weight, gate_weight, query_weight, key_weight, value_weight,
      subtract_share, head_gain[None, :], output_weight)


def fits(S, T, shapes):
    rows = shapes[0][0] // (S * T)
    crows = shapes[1][0] // S
    D = shapes[0][1]
    heads = shapes[8][1] // VALUE
    return (
        S == 4 and T % 2 == 0 and heads == T and rows % (16 * CHUNKS) == 0
        and crows % 16 == 0 and D % (128 * T) == 0 and T >= 4
        and rows * T * D * 8 + T * VALUE * D * 2 < 24 * 1024 * 1024
    )


def solution(mesh):
    in_specs = (
        P(("sp", "tp"), None),
        P("sp", None),
        P("sp"),
        P("sp"),
        P(),
        P("sp", "tp"),
        P("sp", "tp"),
        P("sp", "tp"),
        P(None, "tp"),
        P(None, "tp"),
        P(None, "tp"),
        P("tp"),
        P(),
        P("tp", None),
    )
    out_specs = P(("sp", "tp"), None)
    S, T = mesh.shape["sp"], mesh.shape["tp"]

    def whole(*args):
        if fits(S, T, [a.shape for a in args]):
            body = functools.partial(fused_shards, S, T)
        else:
            body = shards
        return jax.shard_map(
            body, mesh=mesh, in_specs=in_specs, out_specs=out_specs, check_vma=False
        )(*args)

    return whole
```

```python
import functools
import math

import jax
import jax.numpy as jnp
from jax import lax
from jax.experimental import pallas as pl
from jax.experimental.pallas import tpu as pltpu
from jax.sharding import PartitionSpec as P

HEAD = 64
VALUE = 128
GRID_W = 64


norm_eps = 1e-06
head_eps = 1e-05
rope_theta = 10000.0
head_scale = 0.8


def rotary_tables(positions):
    quarter = HEAD // 4
    inverse = rope_theta ** (-2.0 * jnp.arange(quarter, dtype=jnp.float32) / (HEAD // 2))
    row_angle = (positions // GRID_W).astype(jnp.float32)[:, None] * inverse[None, :]
    column_angle = (positions % GRID_W).astype(jnp.float32)[:, None] * inverse[None, :]
    angles = jnp.concatenate([row_angle, row_angle, column_angle, column_angle], axis=-1)
    return (jnp.cos(angles), jnp.sin(angles))


def rotate(vectors, cosine, sine_table):
    quarter = HEAD // 4
    pieces = vectors.reshape(vectors.shape[:-1] + (2, 2, quarter))
    turned = jnp.concatenate([-pieces[..., 1:, :], pieces[..., :1, :]], axis=-2).reshape(
        vectors.shape
    )
    return vectors * cosine[:, None, :] + turned * sine_table[:, None, :]


def modulate(token_rows, gain_row, shift_row, scale_row):
    widened = token_rows.astype(jnp.float32)
    normed = widened * lax.rsqrt(jnp.mean(widened * widened, axis=-1, keepdims=True) + norm_eps)
    return (normed * gain_row * (1.0 + scale_row) + shift_row).astype(jnp.bfloat16)


def shards(
    latents,
    context,
    condition,
    context_condition,
    norm_gain,
    shift_weight,
    scale_weight,
    gate_weight,
    query_weight,
    key_weight,
    value_weight,
    subtract_share,
    head_gain,
    output_weight,
):
    activated = jax.nn.silu(jnp.stack([condition, context_condition])).astype(jnp.bfloat16)
    partial_terms = jnp.stack(
        [
            jnp.dot(activated, matrix, preferred_element_type=jnp.float32)
            for matrix in (shift_weight, scale_weight, gate_weight)
        ]
    )
    summed = lax.psum(partial_terms, "sp")
    full_terms = lax.all_gather(summed, "tp", axis=2, tiled=True)
    shift_terms, scale_terms, gate_terms = (full_terms[0], full_terms[1], full_terms[2])
    pair_weight = jnp.concatenate([key_weight, value_weight], axis=1)
    joined = jnp.concatenate([query_weight, pair_weight], axis=1)
    projected = jnp.dot(
        modulate(
            lax.all_gather(latents, "tp", axis=0, tiled=True),
            norm_gain,
            shift_terms[0],
            scale_terms[0],
        ),
        joined,
        preferred_element_type=jnp.float32,
    )
    local_count = projected.shape[0]
    positions = lax.axis_index("sp") * local_count + jnp.arange(local_count, dtype=jnp.int32)
    cosine, sine_table = rotary_tables(positions)
    queries = rotate(projected[:, :VALUE].reshape(local_count, 2, HEAD), cosine, sine_table)
    queries = queries.reshape(local_count, VALUE).astype(jnp.bfloat16)
    latent_keys = rotate(
        projected[:, VALUE : 2 * VALUE].reshape(local_count, 2, HEAD), cosine, sine_table
    )
    latent_keys = latent_keys.reshape(local_count, VALUE).astype(jnp.bfloat16)
    latent_pairs = jnp.concatenate(
        [latent_keys, projected[:, 2 * VALUE :].astype(jnp.bfloat16)], axis=1
    )
    context_mod = modulate(context, norm_gain, shift_terms[1], scale_terms[1])
    context_pairs = jnp.dot(context_mod, pair_weight, preferred_element_type=jnp.float32).astype(
        jnp.bfloat16
    )
    sent_pairs = jnp.concatenate([latent_pairs, context_pairs], axis=0)
    arrived = lax.all_gather(sent_pairs, "sp", axis=0, tiled=True)
    updated_carry = []
    for which_map in range(2):
        offset = which_map * HEAD
        scores = jnp.einsum(
            "qd,kd->qk",
            queries[:, offset : offset + HEAD],
            arrived[:, offset : offset + HEAD],
            preferred_element_type=jnp.float32,
        ) * HEAD ** (-0.5)
        powers = jnp.exp(scores)
        updated_carry.append(
            jnp.dot(
                powers.astype(jnp.bfloat16), arrived[:, VALUE:], preferred_element_type=jnp.float32
            )
        )
        updated_carry.append(jnp.sum(powers, axis=1, keepdims=True))
    first_sum, first_total, second_sum, second_total = tuple(updated_carry)
    share_value = subtract_share[0]
    difference = first_sum / first_total - share_value * (second_sum / second_total)
    normed = difference * lax.rsqrt(
        jnp.mean(difference * difference, axis=1, keepdims=True) + head_eps
    )
    head_output = (normed * head_gain * head_scale).astype(jnp.bfloat16)
    branch = lax.psum_scatter(
        jnp.dot(head_output, output_weight, preferred_element_type=jnp.float32),
        "tp",
        scatter_dimension=0,
        tiled=True,
    )
    return (latents.astype(jnp.float32) + gate_terms[0] * branch).astype(jnp.bfloat16)


MESH = pl.DeviceIdType.MESH
CHUNKS = 2
FAR_PIECES = 2


def fused_kernel(
    lat_ref, ctx_ref, cond_ref, ccond_ref, gain_ref, shift_hbm, scale_hbm, gate_hbm,
    wq_hbm, wk_hbm, wv_hbm, share_ref, hgain_ref, wo_hbm, out_ref,
    lat, mod, cmod, wqkv, wo, part, terms, tables, queries, kv, ho_send, ho,
    shift_ref, scale_ref, gate_ref, far_send, far_recv,
    load_sem, lat_ss, lat_rs, part_ss, part_rs, term_ss, term_rs,
    kv_ss, kv_rs, ckv_ss, ckv_rs, ho_ss, ho_rs, hx_ss, hx_rs, wo_ss, wo_rs, far_ss, far_rs,
    *, S, T,
):
    f32, bf16 = jnp.float32, jnp.bfloat16
    rows, D = lat_ref.shape
    crows = ctx_ref.shape[0]
    count = rows * T
    width = D // T
    quarter_cols = D // S
    Z = T // 2
    i = lax.axis_index("sp")
    t = lax.axis_index("tp")
    z = lax.div(t, 2)
    y = lax.rem(t, 2)
    mate = t + 1 - 2 * y
    twin = i + 1 - 2 * lax.rem(i, 2)
    across = lax.rem(i + 2, S)
    twin_across = lax.rem(twin + 2, S)
    core = lax.rem(i, 2)
    side = lax.div(i, 2)
    half = D // 2
    pending = []

    def when(cond, action):
        if cond is None:
            action()
        else:
            pl.when(cond)(action)

    def copy(src, dst, ss, rs, sp, tp):
        return pltpu.make_async_remote_copy(
            src_ref=src, dst_ref=dst, send_sem=ss, recv_sem=rs,
            device_id={"sp": sp, "tp": tp}, device_id_type=MESH,
        )

    def send(cond, src, dst, ss, rs, sp, tp):
        made = copy(src, dst, ss, rs, sp, tp)

        def go():
            made.start()

        when(cond, go)
        pending.append((cond, made))

    def arrived(dst, ss, rs):
        copy(dst, dst, ss, rs, twin, t).wait_recv()

    loads = [
        pltpu.make_async_copy(wq_hbm, wqkv.at[:, pl.ds(0, VALUE)], load_sem.at[0]),
        pltpu.make_async_copy(wk_hbm, wqkv.at[:, pl.ds(VALUE, VALUE)], load_sem.at[1]),
        pltpu.make_async_copy(wv_hbm, wqkv.at[:, pl.ds(2 * VALUE, VALUE)], load_sem.at[2]),
        pltpu.make_async_copy(
            wo_hbm.at[:, pl.ds(pl.multiple_of(side * half, half), half)],
            wo.at[pl.ds(t * VALUE, VALUE), :],
            load_sem.at[3],
        ),
        pltpu.make_async_copy(shift_hbm, shift_ref, load_sem.at[4]),
        pltpu.make_async_copy(scale_hbm, scale_ref, load_sem.at[5]),
        pltpu.make_async_copy(gate_hbm, gate_ref, load_sem.at[6]),
    ]

    barrier = pltpu.get_barrier_semaphore()
    for k in range(1, S):
        pl.semaphore_signal(
            barrier, inc=1, device_id={"sp": lax.rem(i + k, S), "tp": t}, device_id_type=MESH
        )
    for k in range(1, T):
        pl.semaphore_signal(
            barrier, inc=1, device_id={"sp": i, "tp": lax.rem(t + k, T)}, device_id_type=MESH
        )
        pl.semaphore_signal(
            barrier, inc=1, device_id={"sp": across, "tp": lax.rem(t + k, T)}, device_id_type=MESH
        )
    for load in loads[4:] + loads[:4]:
        load.start()
    pl.semaphore_wait(barrier, S + 2 * T - 3)

    step = rows // CHUNKS

    def lat_piece(block, c):
        return lat.at[pl.ds(block * rows + c * step, step), :]

    for c in range(CHUNKS):
        own = lat_ref.at[pl.ds(c * step, step), :]
        dst = lat_piece(t, c)
        rs = lat_rs.at[c, t]
        send(z < Z - 1, own, dst, lat_ss.at[c, t, 0], rs, i, t + 2)
        send(z > 0, own, dst, lat_ss.at[c, t, 1], rs, i, t - 2)
        send(None, own, dst, lat_ss.at[c, t, 2], rs, i, mate)

    def lat_stage(d):
        for c in range(CHUNKS):
            for sign in (-1, 1):
                block = t + 2 * d * sign
                here = z - d >= 0 if sign < 0 else z + d < Z
                onward = jnp.logical_and(here, z < Z - 1 if sign < 0 else z > 0)
                piece = lat_piece(block, c)
                rs = lat_rs.at[c, block]

                def come(piece=piece, rs=rs, block=block, c=c):
                    arrived(piece, lat_ss.at[c, block, 0], rs)

                when(here, come)
                send(onward, piece, piece, lat_ss.at[c, block, 0], rs, i, t - 2 * sign)
                send(here, piece, piece, lat_ss.at[c, block, 2], rs, i, mate)

    def silu(v):
        return v / (1.0 + jnp.exp(-v))

    depth = cond_ref.shape[1]
    line = lax.broadcasted_iota(jnp.int32, (8, depth), 0)
    act0 = jnp.broadcast_to(silu(cond_ref[...]), (8, depth))
    act1 = jnp.broadcast_to(silu(ccond_ref[...]), (8, depth))

    def two_lines(first, matrix_ref, with_second):
        left = jnp.where(line == first, act0, 0.0)
        if with_second:
            left = jnp.where(line == first + 1, act1, left)
        return jnp.dot(left.astype(bf16), matrix_ref[...], preferred_element_type=f32)

    for load in loads[4:]:
        load.wait()
    part[pl.ds(i, 1)] = (
        two_lines(0, shift_ref, True) + two_lines(2, scale_ref, True) + two_lines(4, gate_ref, False)
    )[None]
    for k in range(1, S):
        send(None, part.at[i], part.at[i], part_ss.at[k], part_rs.at[i], lax.rem(i + k, S), t)

    lat_stage(1)

    for k in range(1, S):
        peer = lax.rem(i + k, S)
        arrived(part.at[peer], part_ss.at[k], part_rs.at[peer])
    total = part[0]
    for k in range(1, S):
        total = total + part[k]
    terms[pl.ds(t, 1)] = total[None]
    for k in range(1, T):
        send(None, terms.at[t], terms.at[t], term_ss.at[k], term_rs.at[t], i, lax.rem(t + k, T))

    lane = lax.broadcasted_iota(jnp.int32, (count, VALUE), 1)
    place = i * count + lax.broadcasted_iota(jnp.int32, (count, VALUE), 0)
    spot = lax.rem(lane, HEAD)
    quarter = HEAD // 4
    power = lax.rem(spot, quarter).astype(f32) * (-2.0 / (HEAD // 2))
    inverse = jnp.exp(power * math.log(rope_theta))
    along = jnp.where(spot < HEAD // 2, lax.div(place, GRID_W), lax.rem(place, GRID_W))
    angle = along.astype(f32) * inverse
    even = lax.rem(lax.div(spot, quarter), 2) == 0
    tables[0] = jnp.cos(angle)
    tables[1] = jnp.sin(angle)

    def wo_piece(block, share):
        return wo.at[
            pl.ds(block * VALUE, VALUE),
            pl.ds(pl.multiple_of(share * quarter_cols, quarter_cols), quarter_cols),
        ]

    def wo_twin(cond, block):
        piece = wo_piece(block, core)
        send(cond, piece, piece, wo_ss.at[block, 3], wo_rs.at[block, core], twin, t)

    def wo_stage(d):
        for sign in (-1, 1):
            block = t + 2 * d * sign
            here = z - d >= 0 if sign < 0 else z + d < Z
            onward = jnp.logical_and(here, z < Z - 1 if sign < 0 else z > 0)
            piece = wo_piece(block, core)
            rs = wo_rs.at[block, core]

            def come(piece=piece, rs=rs, block=block):
                arrived(piece, wo_ss.at[block, 0], rs)

            when(here, come)
            send(onward, piece, piece, wo_ss.at[block, 0], rs, i, t - 2 * sign)
            send(here, piece, piece, wo_ss.at[block, 2], rs, i, mate)
            wo_twin(here, block)

    def wo_mate(d):
        for sign in (-1, 1) if d else (1,):
            block = mate + 2 * d * sign
            here = None if not d else (z - d >= 0 if sign < 0 else z + d < Z)
            piece = wo_piece(block, core)

            def come(piece=piece, block=block):
                arrived(piece, wo_ss.at[block, 0], wo_rs.at[block, core])

            when(here, come)
            wo_twin(here, block)

    loads[3].wait()
    own_wo = wo_piece(t, core)
    for d in range(2, Z):
        lat_stage(d)
        if d == 2:
            send(z < Z - 1, own_wo, own_wo, wo_ss.at[t, 0], wo_rs.at[t, core], i, t + 2)
            send(z > 0, own_wo, own_wo, wo_ss.at[t, 1], wo_rs.at[t, core], i, t - 2)
    send(None, own_wo, own_wo, wo_ss.at[t, 2], wo_rs.at[t, core], i, mate)

    for k in range(1, T):
        peer = lax.rem(t + k, T)
        arrived(terms.at[peer], term_ss.at[k], term_rs.at[peer])

    def modulate_into(dst, src, first, n, which):
        wide = src[...].astype(f32)
        factor = lax.rsqrt(jnp.mean(wide * wide, axis=-1, keepdims=True) + norm_eps)
        for j in range(T):
            cols = slice(j * width, (j + 1) * width)
            mult = gain_ref[:, cols] * (1.0 + terms[j, 2 + which : 3 + which, :])
            shifted = wide[:, cols] * factor * mult + terms[j, which : which + 1, :]
            dst[pl.ds(first, n), cols] = shifted.astype(bf16)

    for load in loads[:3]:
        load.wait()
    modulate_into(cmod, ctx_ref, 0, crows, 1)
    kv[pl.ds(i, 1), pl.ds(count, crows), :] = jnp.dot(
        cmod[...], wqkv[:, VALUE:], preferred_element_type=f32
    ).astype(bf16)[None]

    def ckv_piece(s):
        return kv.at[s, pl.ds(count, crows), :]

    def kv_piece(s):
        return kv.at[s, pl.ds(0, count), :]

    send(None, ckv_piece(i), ckv_piece(i), ckv_ss.at[0], ckv_rs.at[i], across, t)
    send(None, ckv_piece(i), ckv_piece(i), ckv_ss.at[1], ckv_rs.at[i], twin, t)

    for d in range(Z):
        for sign in (-1, 1) if d else (1,):
            block = mate + 2 * d * sign
            here = None if not d else (z - d >= 0 if sign < 0 else z + d < Z)
            for c in range(CHUNKS):
                def come(block=block, c=c):
                    arrived(lat_piece(block, c), lat_ss.at[c, block, 0], lat_rs.at[c, block])

                when(here, come)
    lat[pl.ds(t * rows, rows), :] = lat_ref[...]
    modulate_into(mod, lat, 0, count, 0)
    projected = jnp.dot(mod[...], wqkv[...], preferred_element_type=f32)

    def rotated(u):
        turned = jnp.where(even, -pltpu.roll(u, VALUE - quarter, 1), pltpu.roll(u, quarter, 1))
        return u * tables[0] + turned * tables[1]

    kv[pl.ds(i, 1), pl.ds(0, count), pl.ds(0, VALUE)] = (
        rotated(projected[:, VALUE : 2 * VALUE]).astype(bf16)[None]
    )
    kv[pl.ds(i, 1), pl.ds(0, count), pl.ds(VALUE, VALUE)] = (
        projected[:, 2 * VALUE :].astype(bf16)[None]
    )
    send(None, kv_piece(i), kv_piece(i), kv_ss.at[0], kv_rs.at[i], across, t)
    send(None, kv_piece(i), kv_piece(i), kv_ss.at[1], kv_rs.at[i], twin, t)
    wo_stage(1)
    arrived(ckv_piece(across), ckv_ss.at[2], ckv_rs.at[across])
    send(None, ckv_piece(across), ckv_piece(across), ckv_ss.at[2], ckv_rs.at[across], twin, t)
    query = rotated(projected[:, :VALUE]).astype(bf16) * jnp.asarray(HEAD ** (-0.5), bf16)
    first_half = lane < HEAD
    zero = jnp.zeros_like(query)
    queries[0:count, :] = jnp.where(first_half, query, zero)
    queries[count:, :] = jnp.where(first_half, zero, query)

    ones = jnp.ones((count + crows, VALUE), bf16)

    def attend(slot):
        rows_kv = kv[slot]
        scores = lax.dot_general(
            queries[...], rows_kv[:, :VALUE], (((1,), (1,)), ((), ())), preferred_element_type=f32
        )
        return jnp.dot(
            jnp.exp(scores).astype(bf16),
            jnp.concatenate([rows_kv[:, VALUE:], ones], axis=1),
            preferred_element_type=f32,
        )

    sums = attend(i)
    arrived(kv_piece(twin), kv_ss.at[2], kv_rs.at[twin])
    arrived(ckv_piece(twin), ckv_ss.at[2], ckv_rs.at[twin])
    sums = sums + attend(twin)
    wo_mate(0)
    wo_stage(2)
    arrived(kv_piece(across), kv_ss.at[2], kv_rs.at[across])
    send(None, kv_piece(across), kv_piece(across), kv_ss.at[2], kv_rs.at[across], twin, t)
    sums = sums + attend(across)
    wo_mate(1)
    arrived(kv_piece(twin_across), kv_ss.at[2], kv_rs.at[twin_across])
    arrived(ckv_piece(twin_across), ckv_ss.at[2], ckv_rs.at[twin_across])
    sums = sums + attend(twin_across)
    ratio = sums[:, :VALUE] / sums[:, VALUE:]
    difference = ratio[:count] - share_ref[0] * ratio[count:]
    normed = difference * lax.rsqrt(
        jnp.mean(difference * difference, axis=1, keepdims=True) + head_eps
    )
    ho_send[...] = (normed * hgain_ref[...] * head_scale).astype(bf16)
    for k in range(1, T):
        peer = lax.rem(t + k, T)
        send(
            None, ho_send.at[pl.ds(peer * rows, rows), :], ho.at[0, t], ho_ss.at[k], ho_rs.at[t], i, peer
        )
    for k in range(T):
        peer = lax.rem(t + k, T)
        send(
            None, ho_send.at[pl.ds(peer * rows, rows), :], ho.at[1, t], hx_ss.at[k], hx_rs.at[t], across, peer
        )
    ho[0, pl.ds(t, 1)] = ho_send[pl.ds(t * rows, rows), :][None]

    for d in range(3, Z):
        wo_stage(d)
    for d in range(2, Z):
        wo_mate(d)
    for k in range(T):
        peer = lax.rem(t + k, T)
        if k:
            arrived(wo_piece(peer, 1 - core), wo_ss.at[peer, 0], wo_rs.at[peer, 1 - core])
            arrived(ho.at[0, peer], ho_ss.at[k], ho_rs.at[peer])
        arrived(ho.at[1, peer], hx_ss.at[k], hx_rs.at[peer])
    heads = jnp.concatenate(
        [jnp.concatenate([ho[which, h] for h in range(T)], axis=1) for which in (1, 0)], axis=0
    )
    near = []
    blocks = T // 2
    per_piece = blocks // FAR_PIECES
    for j in range(blocks):
        gated = terms[pl.ds(side * blocks + j, 1), 4:5, :][0] * jnp.dot(
            heads, wo[:, j * width : (j + 1) * width], preferred_element_type=f32
        )
        far_send[:, j * width : (j + 1) * width] = gated[:rows].astype(bf16)
        near.append(gated[rows:])
        if (j + 1) % per_piece == 0:
            n = j // per_piece
            piece = pl.ds(n * per_piece * width, per_piece * width)
            send(
                None, far_send.at[:, piece], far_recv.at[:, piece], far_ss.at[n], far_rs.at[n], across, t
            )
    for j in range(blocks):
        cols = pl.ds(pl.multiple_of(side * half + j * width, width), width)
        out_ref[:, cols] = (lat_ref[:, cols].astype(f32) + near[j]).astype(bf16)
    for n in range(FAR_PIECES):
        piece = pl.ds(n * per_piece * width, per_piece * width)
        arrived(far_recv.at[:, piece], far_ss.at[n], far_rs.at[n])
        for j in range(n * per_piece, (n + 1) * per_piece):
            cols = pl.ds(pl.multiple_of((1 - side) * half + j * width, width), width)
            out_ref[:, cols] = (
                lat_ref[:, cols].astype(f32)
                + far_recv[:, j * width : (j + 1) * width].astype(f32)
            ).astype(bf16)

    for cond, made in pending:
        def finish(made=made):
            made.wait_send()

        when(cond, finish)


def fused_shards(S, T, *args):
    (latents, context, condition, context_condition, norm_gain, shift_weight, scale_weight,
     gate_weight, query_weight, key_weight, value_weight, subtract_share, head_gain,
     output_weight) = args
    rows, D = latents.shape
    crows = context.shape[0]
    count = rows * T
    bf16, f32 = jnp.bfloat16, jnp.float32
    vmem = pl.BlockSpec(memory_space=pltpu.VMEM)
    hbm = pl.BlockSpec(memory_space=pl.ANY)
    smem = pl.BlockSpec(memory_space=pltpu.SMEM)
    dma = pltpu.SemaphoreType.DMA
    return pl.pallas_call(
        functools.partial(fused_kernel, S=S, T=T),
        out_shape=jax.ShapeDtypeStruct((rows, D), bf16),
        in_specs=[vmem] * 5 + [hbm] * 6 + [smem, vmem, hbm],
        out_specs=vmem,
        scratch_shapes=[
            pltpu.VMEM((count, D), bf16),
            pltpu.VMEM((count, D), bf16),
            pltpu.VMEM((crows, D), bf16),
            pltpu.VMEM((D, 3 * VALUE), bf16),
            pltpu.VMEM((T * VALUE, D // 2), bf16),
            pltpu.VMEM((S, 8, D // T), f32),
            pltpu.VMEM((T, 8, D // T), f32),
            pltpu.VMEM((2, count, VALUE), f32),
            pltpu.VMEM((2 * count, VALUE), bf16),
            pltpu.VMEM((S, count + crows, 2 * VALUE), bf16),
            pltpu.VMEM((count, VALUE), bf16),
            pltpu.VMEM((2, T, rows, VALUE), bf16),
            pltpu.VMEM(shift_weight.shape, bf16),
            pltpu.VMEM(shift_weight.shape, bf16),
            pltpu.VMEM(shift_weight.shape, bf16),
            pltpu.VMEM((rows, D // 2), bf16),
            pltpu.VMEM((rows, D // 2), bf16),
            dma((7,)), dma((CHUNKS, T, 3)), dma((CHUNKS, T)), dma((S,)), dma((S,)),
            dma((T,)), dma((T,)), dma((3,)), dma((S,)), dma((3,)), dma((S,)),
            dma((T,)), dma((T,)), dma((T,)), dma((T,)), dma((T, 4)), dma((T, 2)),
            dma((FAR_PIECES,)), dma((FAR_PIECES,)),
        ],
        compiler_params=pltpu.CompilerParams(
            collective_id=0, has_side_effects=True, vmem_limit_bytes=56 * 1024 * 1024
        ),
    )(latents, context, condition[None, :], context_condition[None, :], norm_gain[None, :],
      shift_weight, scale_weight, gate_weight, query_weight, key_weight, value_weight,
      subtract_share, head_gain[None, :], output_weight)


def fits(S, T, shapes):
    rows = shapes[0][0] // (S * T)
    crows = shapes[1][0] // S
    D = shapes[0][1]
    heads = shapes[8][1] // VALUE
    return (
        S == 4 and T % (2 * FAR_PIECES) == 0 and heads == T and rows % (16 * CHUNKS) == 0
        and crows % 16 == 0 and D % (128 * T) == 0 and T >= 8
        and rows * T * D * 8 + T * VALUE * D * 2 < 24 * 1024 * 1024
    )


def solution(mesh):
    in_specs = (
        P(("sp", "tp"), None),
        P("sp", None),
        P("sp"),
        P("sp"),
        P(),
        P("sp", "tp"),
        P("sp", "tp"),
        P("sp", "tp"),
        P(None, "tp"),
        P(None, "tp"),
        P(None, "tp"),
        P("tp"),
        P(),
        P("tp", None),
    )
    out_specs = P(("sp", "tp"), None)
    S, T = mesh.shape["sp"], mesh.shape["tp"]

    def whole(*args):
        if fits(S, T, [a.shape for a in args]):
            body = functools.partial(fused_shards, S, T)
        else:
            body = shards
        return jax.shard_map(
            body, mesh=mesh, in_specs=in_specs, out_specs=out_specs, check_vma=False
        )(*args)

    return whole
```

```python
import functools
import math

import jax
import jax.numpy as jnp
from jax import lax
from jax.experimental import pallas as pl
from jax.experimental.pallas import tpu as pltpu
from jax.sharding import PartitionSpec as P

HEAD = 64
VALUE = 128
GRID_W = 64


norm_eps = 1e-06
head_eps = 1e-05
rope_theta = 10000.0
head_scale = 0.8


def rotary_tables(positions):
    quarter = HEAD // 4
    inverse = rope_theta ** (-2.0 * jnp.arange(quarter, dtype=jnp.float32) / (HEAD // 2))
    row_angle = (positions // GRID_W).astype(jnp.float32)[:, None] * inverse[None, :]
    column_angle = (positions % GRID_W).astype(jnp.float32)[:, None] * inverse[None, :]
    angles = jnp.concatenate([row_angle, row_angle, column_angle, column_angle], axis=-1)
    return (jnp.cos(angles), jnp.sin(angles))


def rotate(vectors, cosine, sine_table):
    quarter = HEAD // 4
    pieces = vectors.reshape(vectors.shape[:-1] + (2, 2, quarter))
    turned = jnp.concatenate([-pieces[..., 1:, :], pieces[..., :1, :]], axis=-2).reshape(
        vectors.shape
    )
    return vectors * cosine[:, None, :] + turned * sine_table[:, None, :]


def modulate(token_rows, gain_row, shift_row, scale_row):
    widened = token_rows.astype(jnp.float32)
    normed = widened * lax.rsqrt(jnp.mean(widened * widened, axis=-1, keepdims=True) + norm_eps)
    return (normed * gain_row * (1.0 + scale_row) + shift_row).astype(jnp.bfloat16)


def shards(
    latents,
    context,
    condition,
    context_condition,
    norm_gain,
    shift_weight,
    scale_weight,
    gate_weight,
    query_weight,
    key_weight,
    value_weight,
    subtract_share,
    head_gain,
    output_weight,
):
    activated = jax.nn.silu(jnp.stack([condition, context_condition])).astype(jnp.bfloat16)
    partial_terms = jnp.stack(
        [
            jnp.dot(activated, matrix, preferred_element_type=jnp.float32)
            for matrix in (shift_weight, scale_weight, gate_weight)
        ]
    )
    summed = lax.psum(partial_terms, "sp")
    full_terms = lax.all_gather(summed, "tp", axis=2, tiled=True)
    shift_terms, scale_terms, gate_terms = (full_terms[0], full_terms[1], full_terms[2])
    pair_weight = jnp.concatenate([key_weight, value_weight], axis=1)
    joined = jnp.concatenate([query_weight, pair_weight], axis=1)
    projected = jnp.dot(
        modulate(
            lax.all_gather(latents, "tp", axis=0, tiled=True),
            norm_gain,
            shift_terms[0],
            scale_terms[0],
        ),
        joined,
        preferred_element_type=jnp.float32,
    )
    local_count = projected.shape[0]
    positions = lax.axis_index("sp") * local_count + jnp.arange(local_count, dtype=jnp.int32)
    cosine, sine_table = rotary_tables(positions)
    queries = rotate(projected[:, :VALUE].reshape(local_count, 2, HEAD), cosine, sine_table)
    queries = queries.reshape(local_count, VALUE).astype(jnp.bfloat16)
    latent_keys = rotate(
        projected[:, VALUE : 2 * VALUE].reshape(local_count, 2, HEAD), cosine, sine_table
    )
    latent_keys = latent_keys.reshape(local_count, VALUE).astype(jnp.bfloat16)
    latent_pairs = jnp.concatenate(
        [latent_keys, projected[:, 2 * VALUE :].astype(jnp.bfloat16)], axis=1
    )
    context_mod = modulate(context, norm_gain, shift_terms[1], scale_terms[1])
    context_pairs = jnp.dot(context_mod, pair_weight, preferred_element_type=jnp.float32).astype(
        jnp.bfloat16
    )
    sent_pairs = jnp.concatenate([latent_pairs, context_pairs], axis=0)
    arrived = lax.all_gather(sent_pairs, "sp", axis=0, tiled=True)
    updated_carry = []
    for which_map in range(2):
        offset = which_map * HEAD
        scores = jnp.einsum(
            "qd,kd->qk",
            queries[:, offset : offset + HEAD],
            arrived[:, offset : offset + HEAD],
            preferred_element_type=jnp.float32,
        ) * HEAD ** (-0.5)
        powers = jnp.exp(scores)
        updated_carry.append(
            jnp.dot(
                powers.astype(jnp.bfloat16), arrived[:, VALUE:], preferred_element_type=jnp.float32
            )
        )
        updated_carry.append(jnp.sum(powers, axis=1, keepdims=True))
    first_sum, first_total, second_sum, second_total = tuple(updated_carry)
    share_value = subtract_share[0]
    difference = first_sum / first_total - share_value * (second_sum / second_total)
    normed = difference * lax.rsqrt(
        jnp.mean(difference * difference, axis=1, keepdims=True) + head_eps
    )
    head_output = (normed * head_gain * head_scale).astype(jnp.bfloat16)
    branch = lax.psum_scatter(
        jnp.dot(head_output, output_weight, preferred_element_type=jnp.float32),
        "tp",
        scatter_dimension=0,
        tiled=True,
    )
    return (latents.astype(jnp.float32) + gate_terms[0] * branch).astype(jnp.bfloat16)


MESH = pl.DeviceIdType.MESH
CHUNKS = 4
WEIGHT_CHUNKS = 2
FAR_PIECES = 2


def fused_kernel(
    lat_ref, ctx_ref, cond_ref, ccond_ref, gain_ref, shift_hbm, scale_hbm, gate_hbm,
    wq_hbm, wk_hbm, wv_hbm, share_ref, hgain_ref, wo_hbm, out_ref,
    lat, mod, cmod, wqkv, wo, part, terms, tables, queries, kv, ho_send, ho,
    shift_ref, scale_ref, gate_ref, far_send, far_recv,
    load_sem, lat_ss, lat_rs, lat_yss, lat_yrs, part_ss, part_rs, term_ss, term_rs,
    kv_ss, kv_rs, ckv_ss, ckv_rs, ho_ss, ho_rs, hx_ss, hx_rs, wo_ss, wo_rs, wo_mrs, wo_yss, wo_tss, wo_trs, far_ss, far_rs,
    *, S, T,
):
    f32, bf16 = jnp.float32, jnp.bfloat16
    rows, D = lat_ref.shape
    crows = ctx_ref.shape[0]
    count = rows * T
    width = D // T
    quarter_cols = D // S
    Z = T // 2
    i = lax.axis_index("sp")
    t = lax.axis_index("tp")
    z = lax.div(t, 2)
    y = lax.rem(t, 2)
    mate = t + 1 - 2 * y
    even_layer = lax.rem(z, 2) == 0
    paired = t + 2 - 4 * lax.rem(z, 2)
    twin = i + 1 - 2 * lax.rem(i, 2)
    across = lax.rem(i + 2, S)
    twin_across = lax.rem(twin + 2, S)
    core = lax.rem(i, 2)
    side = lax.div(i, 2)
    half = D // 2
    pending = []
    late = []

    def when(cond, action):
        if cond is None:
            action()
        else:
            pl.when(cond)(action)

    def copy(src, dst, ss, rs, sp, tp):
        return pltpu.make_async_remote_copy(
            src_ref=src, dst_ref=dst, send_sem=ss, recv_sem=rs,
            device_id={"sp": sp, "tp": tp}, device_id_type=MESH,
        )

    def send(cond, src, dst, ss, rs, sp, tp, tracked=True):
        made = copy(src, dst, ss, rs, sp, tp)

        def go():
            made.start()

        when(cond, go)
        if tracked:
            pending.append((cond, made))

    def drain():
        for cond, made in pending:
            def finish(made=made):
                made.wait_send()

            when(cond, finish)
        pending.clear()

    def sent_all(view, ss):
        copy(view, view, ss, ss, twin, t).wait_send()

    def arrived(dst, ss, rs):
        copy(dst, dst, ss, rs, twin, t).wait_recv()

    loads = [
        pltpu.make_async_copy(wq_hbm, wqkv.at[:, pl.ds(0, VALUE)], load_sem.at[0]),
        pltpu.make_async_copy(wk_hbm, wqkv.at[:, pl.ds(VALUE, VALUE)], load_sem.at[1]),
        pltpu.make_async_copy(wv_hbm, wqkv.at[:, pl.ds(2 * VALUE, VALUE)], load_sem.at[2]),
        pltpu.make_async_copy(
            wo_hbm.at[:, pl.ds(pl.multiple_of(side * half, half), half)],
            wo.at[pl.ds(t * VALUE, VALUE), :],
            load_sem.at[3],
        ),
        pltpu.make_async_copy(shift_hbm, shift_ref, load_sem.at[4]),
        pltpu.make_async_copy(scale_hbm, scale_ref, load_sem.at[5]),
        pltpu.make_async_copy(gate_hbm, gate_ref, load_sem.at[6]),
    ]

    barrier = pltpu.get_barrier_semaphore()
    for k in range(1, S):
        pl.semaphore_signal(
            barrier, inc=1, device_id={"sp": lax.rem(i + k, S), "tp": t}, device_id_type=MESH
        )
    for k in range(1, T):
        pl.semaphore_signal(
            barrier, inc=1, device_id={"sp": i, "tp": lax.rem(t + k, T)}, device_id_type=MESH
        )
        pl.semaphore_signal(
            barrier, inc=1, device_id={"sp": across, "tp": lax.rem(t + k, T)}, device_id_type=MESH
        )
    for load in loads[4:] + loads[:4]:
        load.start()
    pl.semaphore_wait(barrier, S + 2 * T - 3)

    step = D // CHUNKS

    def lat_piece(block, c):
        return lat.at[pl.ds(block * rows, rows), pl.ds(c * step, step)]

    for c in range(CHUNKS):
        own = lat_ref.at[:, pl.ds(c * step, step)]
        dst = lat_piece(t, c)
        send(z < Z - 1, own, dst, lat_ss.at[c, z], lat_rs.at[c, z], i, t + 2)
        send(z > 0, own, dst, lat_ss.at[c, Z], lat_rs.at[c, z], i, t - 2)
        rs = lat_rs.at[c, Z] if c >= CHUNKS // 2 else lat_yrs.at[0]
        send(None, own, dst, lat_yss.at[0], rs, i, mate, False)

    def lat_stage(d):
        for c in range(CHUNKS):
            for sign in (-1, 1):
                block = t + 2 * d * sign
                here = z - d >= 0 if sign < 0 else z + d < Z
                onward = jnp.logical_and(here, z < Z - 1 if sign < 0 else z > 0)
                piece = lat_piece(block, c)
                layer = z + d * sign
                rs = lat_rs.at[c, layer]

                def come(piece=piece, rs=rs):
                    arrived(piece, lat_yss.at[0], rs)

                when(here, come)
                send(onward, piece, piece, lat_ss.at[c, layer], rs, i, t - 2 * sign)
                over = here
                if d == 1 and c >= CHUNKS // 2:
                    over = jnp.logical_and(here, even_layer if sign < 0 else jnp.logical_not(even_layer))
                send(over, piece, piece, lat_yss.at[0], lat_yrs.at[0], i, mate, False)

    def lat_cross():
        for c in range(CHUNKS // 2, CHUNKS):
            piece = lat_piece(mate, c)
            arrived(piece, lat_yss.at[0], lat_rs.at[c, Z])
            send(None, piece, piece, lat_ss.at[c, Z + 1], lat_yrs.at[0], i, paired)

    def silu(v):
        return v / (1.0 + jnp.exp(-v))

    depth = cond_ref.shape[1]
    line = lax.broadcasted_iota(jnp.int32, (8, depth), 0)
    act0 = jnp.broadcast_to(silu(cond_ref[...]), (8, depth))
    act1 = jnp.broadcast_to(silu(ccond_ref[...]), (8, depth))

    def two_lines(first, matrix_ref, with_second):
        left = jnp.where(line == first, act0, 0.0)
        if with_second:
            left = jnp.where(line == first + 1, act1, left)
        return jnp.dot(left.astype(bf16), matrix_ref[...], preferred_element_type=f32)

    for load in loads[4:]:
        load.wait()
    part[pl.ds(i, 1)] = (
        two_lines(0, shift_ref, True) + two_lines(2, scale_ref, True) + two_lines(4, gate_ref, False)
    )[None]
    for k in range(1, S):
        send(None, part.at[i], part.at[i], part_ss.at[0], part_rs.at[0], lax.rem(i + k, S), t, False)

    lat_stage(1)
    lat_cross()

    arrived(part.at[pl.ds(0, S - 1)], part_ss.at[0], part_rs.at[0])
    total = part[0]
    for k in range(1, S):
        total = total + part[k]
    terms[pl.ds(t, 1)] = total[None]
    for k in range(1, T):
        send(
            None, terms.at[t], terms.at[t], term_ss.at[0], term_rs.at[0], i, lax.rem(t + k, T), False
        )

    lane = lax.broadcasted_iota(jnp.int32, (count, VALUE), 1)
    place = i * count + lax.broadcasted_iota(jnp.int32, (count, VALUE), 0)
    spot = lax.rem(lane, HEAD)
    quarter = HEAD // 4
    power = lax.rem(spot, quarter).astype(f32) * (-2.0 / (HEAD // 2))
    inverse = jnp.exp(power * math.log(rope_theta))
    along = jnp.where(spot < HEAD // 2, lax.div(place, GRID_W), lax.rem(place, GRID_W))
    angle = along.astype(f32) * inverse
    even = lax.rem(lax.div(spot, quarter), 2) == 0
    tables[0] = jnp.cos(angle)
    tables[1] = jnp.sin(angle)

    weight_step = VALUE // WEIGHT_CHUNKS

    def wo_piece(block, share, w):
        return wo.at[
            pl.ds(block * VALUE + w * weight_step, weight_step),
            pl.ds(pl.multiple_of(share * quarter_cols, quarter_cols), quarter_cols),
        ]

    def wo_arrive(cond, block, rs, w):
        def come():
            arrived(wo_piece(block, core, w), wo_yss.at[0], rs)

        when(cond, come)

    def wo_send(cond, block, ss, rs, w, sp, tp, tracked=True):
        piece = wo_piece(block, core, w)
        send(cond, piece, piece, ss, rs, sp, tp, tracked)
        if tracked:
            late.append(pending.pop())

    def wo_twin(cond, block, w):
        wo_send(cond, block, wo_tss.at[0], wo_trs.at[0], w, twin, t, False)

    def wo_stage(d):
        for w in range(WEIGHT_CHUNKS):
            for sign in (-1, 1):
                layer = z + d * sign
                block = t + 2 * d * sign
                here = z - d >= 0 if sign < 0 else z + d < Z
                onward = jnp.logical_and(here, z < Z - 1 if sign < 0 else z > 0)
                wo_arrive(here, block, wo_rs.at[w, layer], w)
                wo_send(onward, block, wo_ss.at[w, layer], wo_rs.at[w, layer], w, i, t - 2 * sign)
                over = here
                if d == 1 and w >= WEIGHT_CHUNKS // 2:
                    over = jnp.logical_and(here, even_layer if sign < 0 else jnp.logical_not(even_layer))
                wo_send(over, block, wo_yss.at[0], wo_mrs.at[w, layer], w, i, mate, False)
                wo_twin(here, block, w)

    def wo_mate(d):
        for w in range(WEIGHT_CHUNKS):
            for sign in (-1, 1) if d else (1,):
                layer = z + d * sign
                block = mate + 2 * d * sign
                here = None if not d else (z - d >= 0 if sign < 0 else z + d < Z)
                wo_arrive(here, block, wo_mrs.at[w, layer], w)
                if not d and w >= WEIGHT_CHUNKS // 2:
                    wo_send(None, block, wo_ss.at[w, Z + 1], wo_mrs.at[w, z], w, i, paired)
                wo_twin(here, block, w)

    loads[3].wait()
    for d in range(2, Z):
        lat_stage(d)
        if d == 2:
            for w in range(WEIGHT_CHUNKS):
                wo_send(z < Z - 1, t, wo_ss.at[w, z], wo_rs.at[w, z], w, i, t + 2)
                wo_send(z > 0, t, wo_ss.at[w, Z], wo_rs.at[w, z], w, i, t - 2)
    for w in range(WEIGHT_CHUNKS):
        wo_send(None, t, wo_yss.at[0], wo_mrs.at[w, z], w, i, mate, False)

    arrived(terms.at[pl.ds(0, T - 1)], term_ss.at[0], term_rs.at[0])

    def modulate_into(dst, src, first, n, which):
        wide = src[...].astype(f32)
        factor = lax.rsqrt(jnp.mean(wide * wide, axis=-1, keepdims=True) + norm_eps)
        for j in range(T):
            cols = slice(j * width, (j + 1) * width)
            mult = gain_ref[:, cols] * (1.0 + terms[j, 2 + which : 3 + which, :])
            shifted = wide[:, cols] * factor * mult + terms[j, which : which + 1, :]
            dst[pl.ds(first, n), cols] = shifted.astype(bf16)

    for load in loads[:3]:
        load.wait()
    modulate_into(cmod, ctx_ref, 0, crows, 1)
    kv[pl.ds(i, 1), pl.ds(count, crows), :] = jnp.dot(
        cmod[...], wqkv[:, VALUE:], preferred_element_type=f32
    ).astype(bf16)[None]

    def ckv_piece(s):
        return kv.at[s, pl.ds(count, crows), :]

    def kv_piece(s):
        return kv.at[s, pl.ds(0, count), :]

    send(None, ckv_piece(i), ckv_piece(i), ckv_ss.at[0], ckv_rs.at[i], across, t)
    send(None, ckv_piece(i), ckv_piece(i), ckv_ss.at[1], ckv_rs.at[i], twin, t)

    over_rows = Z * rows - rows // 2
    arrived(lat.at[pl.ds(0, over_rows), :], lat_yss.at[0], lat_yrs.at[0])
    lat[pl.ds(t * rows, rows), :] = lat_ref[...]
    modulate_into(mod, lat, 0, count, 0)
    projected = jnp.dot(mod[...], wqkv[...], preferred_element_type=f32)

    def rotated(u):
        turned = jnp.where(even, -pltpu.roll(u, VALUE - quarter, 1), pltpu.roll(u, quarter, 1))
        return u * tables[0] + turned * tables[1]

    kv[pl.ds(i, 1), pl.ds(0, count), pl.ds(0, VALUE)] = (
        rotated(projected[:, VALUE : 2 * VALUE]).astype(bf16)[None]
    )
    kv[pl.ds(i, 1), pl.ds(0, count), pl.ds(VALUE, VALUE)] = (
        projected[:, 2 * VALUE :].astype(bf16)[None]
    )
    send(None, kv_piece(i), kv_piece(i), kv_ss.at[0], kv_rs.at[i], across, t)
    send(None, kv_piece(i), kv_piece(i), kv_ss.at[1], kv_rs.at[i], twin, t)
    arrived(ckv_piece(across), ckv_ss.at[2], ckv_rs.at[across])
    send(None, ckv_piece(across), ckv_piece(across), ckv_ss.at[2], ckv_rs.at[across], twin, t)
    query = rotated(projected[:, :VALUE]).astype(bf16) * jnp.asarray(HEAD ** (-0.5), bf16)
    first_half = lane < HEAD
    zero = jnp.zeros_like(query)
    queries[0:count, :] = jnp.where(first_half, query, zero)
    queries[count:, :] = jnp.where(first_half, zero, query)

    ones = jnp.ones((count + crows, VALUE), bf16)

    def attend(slot):
        rows_kv = kv[slot]
        scores = lax.dot_general(
            queries[...], rows_kv[:, :VALUE], (((1,), (1,)), ((), ())), preferred_element_type=f32
        )
        return jnp.dot(
            jnp.exp(scores).astype(bf16),
            jnp.concatenate([rows_kv[:, VALUE:], ones], axis=1),
            preferred_element_type=f32,
        )

    sums = attend(i)
    wo_stage(1)
    wo_mate(0)
    arrived(kv_piece(twin), kv_ss.at[2], kv_rs.at[twin])
    arrived(ckv_piece(twin), ckv_ss.at[2], ckv_rs.at[twin])
    sums = sums + attend(twin)
    arrived(kv_piece(across), kv_ss.at[2], kv_rs.at[across])
    send(None, kv_piece(across), kv_piece(across), kv_ss.at[2], kv_rs.at[across], twin, t)
    wo_stage(2)
    sums = sums + attend(across)
    arrived(kv_piece(twin_across), kv_ss.at[2], kv_rs.at[twin_across])
    arrived(ckv_piece(twin_across), ckv_ss.at[2], ckv_rs.at[twin_across])
    sums = sums + attend(twin_across)
    ratio = sums[:, :VALUE] / sums[:, VALUE:]
    difference = ratio[:count] - share_ref[0] * ratio[count:]
    normed = difference * lax.rsqrt(
        jnp.mean(difference * difference, axis=1, keepdims=True) + head_eps
    )
    ho_send[...] = (normed * hgain_ref[...] * head_scale).astype(bf16)
    for k in range(1, T):
        peer = lax.rem(t + k, T)
        send(
            None, ho_send.at[pl.ds(peer * rows, rows), :], ho.at[0, t], ho_ss.at[0], ho_rs.at[0], i, peer, False
        )
    for k in range(T):
        peer = lax.rem(t + k, T)
        send(
            None, ho_send.at[pl.ds(peer * rows, rows), :], ho.at[1, t], hx_ss.at[0], hx_rs.at[0], across, peer, False
        )
    ho[0, pl.ds(t, 1)] = ho_send[pl.ds(t * rows, rows), :][None]

    for d in range(3, Z):
        wo_stage(d)
    drain()
    sent_all(lat.at[pl.ds(0, over_rows), :], lat_yss.at[0])
    sent_all(part.at[pl.ds(0, S - 1)], part_ss.at[0])
    sent_all(terms.at[pl.ds(0, T - 1)], term_ss.at[0])
    for d in range(1, Z):
        wo_mate(d)
    twin_rows = (T - 1) * VALUE
    twin_view = wo.at[pl.ds(0, twin_rows), pl.ds(0, quarter_cols)]
    arrived(twin_view, wo_tss.at[0], wo_trs.at[0])
    pending[:] = late
    drain()
    sent_all(wo.at[pl.ds(0, Z * VALUE - weight_step), pl.ds(0, quarter_cols)], wo_yss.at[0])
    arrived(ho.at[0, pl.ds(0, T - 1)], ho_ss.at[0], ho_rs.at[0])
    arrived(ho.at[1], hx_ss.at[0], hx_rs.at[0])
    heads = jnp.concatenate(
        [jnp.concatenate([ho[which, h] for h in range(T)], axis=1) for which in (1, 0)], axis=0
    )
    near = []
    blocks = T // 2
    per_piece = blocks // FAR_PIECES
    for j in range(blocks):
        gated = terms[pl.ds(side * blocks + j, 1), 4:5, :][0] * jnp.dot(
            heads, wo[:, j * width : (j + 1) * width], preferred_element_type=f32
        )
        far_send[:, j * width : (j + 1) * width] = gated[:rows].astype(bf16)
        near.append(gated[rows:])
        if (j + 1) % per_piece == 0:
            n = j // per_piece
            piece = pl.ds(n * per_piece * width, per_piece * width)
            send(
                None, far_send.at[:, piece], far_recv.at[:, piece], far_ss.at[n], far_rs.at[n], across, t
            )
    for j in range(blocks):
        cols = pl.ds(pl.multiple_of(side * half + j * width, width), width)
        out_ref[:, cols] = (lat_ref[:, cols].astype(f32) + near[j]).astype(bf16)
    sent_all(twin_view, wo_tss.at[0])
    sent_all(ho.at[0, pl.ds(0, T - 1)], ho_ss.at[0])
    sent_all(ho.at[1], hx_ss.at[0])
    for n in range(FAR_PIECES):
        piece = pl.ds(n * per_piece * width, per_piece * width)
        arrived(far_recv.at[:, piece], far_ss.at[n], far_rs.at[n])
        for j in range(n * per_piece, (n + 1) * per_piece):
            cols = pl.ds(pl.multiple_of((1 - side) * half + j * width, width), width)
            out_ref[:, cols] = (
                lat_ref[:, cols].astype(f32)
                + far_recv[:, j * width : (j + 1) * width].astype(f32)
            ).astype(bf16)

    drain()


def fused_shards(S, T, *args):
    (latents, context, condition, context_condition, norm_gain, shift_weight, scale_weight,
     gate_weight, query_weight, key_weight, value_weight, subtract_share, head_gain,
     output_weight) = args
    rows, D = latents.shape
    crows = context.shape[0]
    count = rows * T
    bf16, f32 = jnp.bfloat16, jnp.float32
    vmem = pl.BlockSpec(memory_space=pltpu.VMEM)
    hbm = pl.BlockSpec(memory_space=pl.ANY)
    smem = pl.BlockSpec(memory_space=pltpu.SMEM)
    dma = pltpu.SemaphoreType.DMA
    return pl.pallas_call(
        functools.partial(fused_kernel, S=S, T=T),
        out_shape=jax.ShapeDtypeStruct((rows, D), bf16),
        in_specs=[vmem] * 5 + [hbm] * 6 + [smem, vmem, hbm],
        out_specs=vmem,
        scratch_shapes=[
            pltpu.VMEM((count, D), bf16),
            pltpu.VMEM((count, D), bf16),
            pltpu.VMEM((crows, D), bf16),
            pltpu.VMEM((D, 3 * VALUE), bf16),
            pltpu.VMEM((T * VALUE, D // 2), bf16),
            pltpu.VMEM((S, 8, D // T), f32),
            pltpu.VMEM((T, 8, D // T), f32),
            pltpu.VMEM((2, count, VALUE), f32),
            pltpu.VMEM((2 * count, VALUE), bf16),
            pltpu.VMEM((S, count + crows, 2 * VALUE), bf16),
            pltpu.VMEM((count, VALUE), bf16),
            pltpu.VMEM((2, T, rows, VALUE), bf16),
            pltpu.VMEM(shift_weight.shape, bf16),
            pltpu.VMEM(shift_weight.shape, bf16),
            pltpu.VMEM(shift_weight.shape, bf16),
            pltpu.VMEM((rows, D // 2), bf16),
            pltpu.VMEM((rows, D // 2), bf16),
            dma((7,)), dma((CHUNKS, T // 2 + 2)), dma((CHUNKS, T // 2 + 1)), dma((1,)), dma((1,)),
            dma((1,)), dma((1,)), dma((1,)), dma((1,)),
            dma((3,)), dma((S,)), dma((3,)), dma((S,)),
            dma((1,)), dma((1,)), dma((1,)), dma((1,)),
            dma((WEIGHT_CHUNKS, T // 2 + 2)), dma((WEIGHT_CHUNKS, T // 2)),
            dma((WEIGHT_CHUNKS, T // 2)), dma((1,)), dma((1,)), dma((1,)),
            dma((FAR_PIECES,)), dma((FAR_PIECES,)),
        ],
        compiler_params=pltpu.CompilerParams(
            collective_id=0, has_side_effects=True, vmem_limit_bytes=56 * 1024 * 1024
        ),
    )(latents, context, condition[None, :], context_condition[None, :], norm_gain[None, :],
      shift_weight, scale_weight, gate_weight, query_weight, key_weight, value_weight,
      subtract_share, head_gain[None, :], output_weight)


def fits(S, T, shapes):
    rows = shapes[0][0] // (S * T)
    crows = shapes[1][0] // S
    D = shapes[0][1]
    heads = shapes[8][1] // VALUE
    return (
        S == 4 and T % (2 * FAR_PIECES) == 0 and heads == T and rows % 16 == 0
        and crows % 16 == 0 and D % (128 * T) == 0 and D % (128 * CHUNKS) == 0 and T >= 8
        and rows * T * D * 8 + T * VALUE * D * 2 < 24 * 1024 * 1024
    )


def solution(mesh):
    in_specs = (
        P(("sp", "tp"), None),
        P("sp", None),
        P("sp"),
        P("sp"),
        P(),
        P("sp", "tp"),
        P("sp", "tp"),
        P("sp", "tp"),
        P(None, "tp"),
        P(None, "tp"),
        P(None, "tp"),
        P("tp"),
        P(),
        P("tp", None),
    )
    out_specs = P(("sp", "tp"), None)
    S, T = mesh.shape["sp"], mesh.shape["tp"]

    def whole(*args):
        if fits(S, T, [a.shape for a in args]):
            body = functools.partial(fused_shards, S, T)
        else:
            body = shards
        return jax.shard_map(
            body, mesh=mesh, in_specs=in_specs, out_specs=out_specs, check_vma=False
        )(*args)

    return whole
```
